128 devices in a mesh: ep: 16 (over z, x), tp: 8 (over y, core).
Axes of the slice: x: 4, y: 4, z: 4, core: 2. Of those that a mesh axis runs over, the one named last changes fastest.
Arguments:
- out_gate: bfloat16 [32768, 1024], P('ep', 'tp'), may hold values from -6 to 6
- in_gate: bfloat16 [32768, 1024], P('ep', 'tp'), may hold values from -6 to 6
- conv_input: bfloat16 [32768, 1024], P('ep', 'tp'), may hold values from -6 to 6
- conv_taps: float32 [3, 1024], P(None, 'tp'), may hold values from -4 to 4
- group_gain: float32 [1024], P('tp'), may hold values from 0.1 to 1.9
- mix_out_w: bfloat16 [1024, 2048], replicated, may hold values from -0.1875 to 0.1875
- moe_in: bfloat16 [32768, 2048], P(('ep', 'tp')), may hold values from -6 to 6
- moe_gain: float32 [2048], replicated, may hold values from 0.1 to 1.9
- route_ids: int32 [32768, 2], P(('ep', 'tp')), may hold values from 0 to 127, as said below
- route_weight: float32 [32768, 2], P(('ep', 'tp')), may hold values from 0.1 to 1
- gate_w: bfloat16 [128, 2048, 1024], P(('ep', 'tp')), may hold values from -0.125 to 0.125
- up_w: bfloat16 [128, 2048, 1024], P(('ep', 'tp')), may hold values from -0.125 to 0.125
- down_w: bfloat16 [128, 1024, 2048], P(('ep', 'tp')), may hold values from -0.1875 to 0.1875
Outputs:
- mixed: bfloat16 [32768, 2048], P(('ep', 'tp'))
- moe_out: bfloat16 [32768, 2048], P(('ep', 'tp'))
The draws below stay inside these ranges and needn't reach their ends.
Inputs may be any that keep to these rules, and one draw needn't show every extreme that they name: `route_ids`: the two numbers of a row are different experts of one group: group g holds experts g * 8 to g * 8 + 7. The rows of one device (aligned blocks of 256 rows) name each group in exactly 16 rows and each expert in exactly 4 rows.
All inputs are finite; a program needn't handle non-finite values.
Results may differ from the reference program's by a relative error of at most 0.0071.
Values may be sent and summed in bfloat16 or wider, within the bound.
A program may use at most 128 MiB of HBM per device.

```python
import jax
import jax.numpy as jnp
from jax import lax

D = 2048
CC = 1024
GROUP_CH = 64
TAPS = 3
FE = 1024
TOK_B = 256
GROUPS = 16
EXP_GROUP = 8
EXPERTS = 128
TOKENS_A = 32768
TOKENS_B = 32768


def draw_route_ids(key, part):
    block_count = TOKENS_B // TOK_B
    per_group = TOK_B // GROUPS
    block_keys = jax.random.split(jax.random.fold_in(key, 11), block_count)

    def one_block(block_key):
        order_key, label_key = jax.random.split(block_key)
        slot_of = jax.random.permutation(order_key, TOK_B).astype(jnp.int32)
        group_of = slot_of // per_group
        inner_slot = slot_of % per_group
        first_pick = inner_slot % EXP_GROUP
        shift_by = 1 + inner_slot // EXP_GROUP % (EXP_GROUP - 1)
        second_pick = (first_pick + shift_by) % EXP_GROUP
        label_keys = jax.random.split(label_key, GROUPS)
        labels = jax.vmap(lambda one_key: jax.random.permutation(one_key, EXP_GROUP))(label_keys).astype(jnp.int32)
        first_id = group_of * EXP_GROUP + labels[group_of, first_pick]
        second_id = group_of * EXP_GROUP + labels[group_of, second_pick]
        return jnp.stack([first_id, second_id], axis=1)
    return jax.vmap(one_block)(block_keys).reshape(TOKENS_B, 2).astype(jnp.int32)


def block_scale(own_key, extent, cuts, low, largest):
    loudness, own = 1.0, jax.random.fold_in(own_key, 6)
    for dim, parts in cuts:
        draws = jnp.exp(jax.random.uniform(jax.random.fold_in(own, dim), (parts,), jnp.float32, low / len(cuts), largest / len(cuts)))
        loudness = loudness * jnp.repeat(draws, extent[dim] // parts).reshape([-1 if axis == dim else 1 for axis in range(len(extent))])
    return loudness


def centred(own_key, shape, deviation, bound, pieces=(), dtype=jnp.bfloat16):
    drawn = deviation * jax.random.normal(own_key, shape, jnp.float32)
    if pieces:
        drawn = drawn * block_scale(own_key, shape, pieces, -0.22, 0.18)
    return jnp.clip(drawn, -bound, bound).astype(dtype)


def setup_inputs(seed: int = 0) -> dict:
    keys = jax.random.split(jax.random.key(seed), 14)
    return {
        "out_gate": centred(keys[0], (TOKENS_A, CC), 1.0, 6.0, ((0, 16), (1, 8))),
        "in_gate": centred(keys[1], (TOKENS_A, CC), 1.0, 6.0, ((0, 16), (1, 8))),
        "conv_input": centred(keys[2], (TOKENS_A, CC), 1.0, 6.0, ((0, 16), (1, 8))),
        "conv_taps": centred(keys[3], (TAPS, CC), 0.577, 4.0, ((1, 8),), jnp.float32),
        "group_gain": jnp.clip(1.0 + 0.18 * jax.random.normal(keys[4], (CC,), jnp.float32), 0.1, 1.9),
        "mix_out_w": centred(keys[5], (CC, D), CC ** -0.5, 0.1875),
        "moe_in": centred(keys[6], (TOKENS_B, D), 1.0, 6.0, ((0, 128),)),
        "moe_gain": jnp.clip(1.0 + 0.18 * jax.random.normal(keys[7], (D,), jnp.float32), 0.1, 1.9),
        "route_ids": draw_route_ids(jax.random.fold_in(keys[13], 71), 0),
        "route_weight": jnp.clip(0.1 + 0.9 * jax.random.uniform(keys[9], (TOKENS_B, 2), jnp.float32) ** block_scale(keys[9], (TOKENS_B, 2), ((0, 128),), -0.2, 0.2), 0.1, 1.0),
        "gate_w": centred(keys[10], (EXPERTS, D, FE), D ** -0.5, 0.125, ((0, 128),)),
        "up_w": centred(keys[11], (EXPERTS, D, FE), D ** -0.5, 0.125, ((0, 128),)),
        "down_w": centred(keys[12], (EXPERTS, FE, D), FE ** -0.5, 0.1875, ((0, 128),)),
    }


def conv_mixer(out_gate, in_gate, conv_input, conv_taps, group_gain, mix_out_w):
    product = in_gate.astype(jnp.float32) * conv_input.astype(jnp.float32)
    length = product.shape[0]
    padded = jnp.pad(product, ((TAPS - 1, 0), (0, 0)))
    convolved = jnp.zeros_like(product)
    for tap in range(TAPS):
        convolved = convolved + conv_taps[tap] * padded[tap:tap + length]
    gated = out_gate.astype(jnp.float32) * convolved
    grouped = gated.reshape(length, CC // GROUP_CH, GROUP_CH)
    inv_rms = lax.rsqrt(lax.optimization_barrier(jnp.mean(grouped * grouped, axis=-1, keepdims=True)) + 1e-06)
    normed = ((grouped * inv_rms).reshape(length, CC) * group_gain).astype(jnp.bfloat16)
    return jnp.dot(normed, mix_out_w, preferred_element_type=jnp.float32).astype(jnp.bfloat16)

def expert_rows(inputs, w_gate, w_up, w_down):
    gate_part = jnp.dot(inputs, w_gate, preferred_element_type=jnp.float32)
    up_part = jnp.dot(inputs, w_up, preferred_element_type=jnp.float32)
    hidden = (jax.nn.silu(gate_part) * up_part).astype(jnp.bfloat16)
    return jnp.dot(hidden, w_down, preferred_element_type=jnp.float32).astype(jnp.bfloat16)

def reference(out_gate, in_gate, conv_input, conv_taps, group_gain, mix_out_w, moe_in, moe_gain, route_ids, route_weight, gate_w, up_w, down_w):
    mixed = conv_mixer(out_gate, in_gate, conv_input, conv_taps, group_gain, mix_out_w)
    wide_in = moe_in.astype(jnp.float32)
    inv_rms = lax.rsqrt(lax.optimization_barrier(jnp.mean(wide_in * wide_in, axis=-1, keepdims=True)) + 1e-06)
    expert_in = (wide_in * inv_rms * moe_gain).astype(jnp.bfloat16)
    flat_ids = route_ids.reshape(-1).astype(jnp.int32)
    sort_order = jnp.argsort(flat_ids).astype(jnp.int32)
    per_expert = flat_ids.shape[0] // EXPERTS
    tokens_of = (sort_order // 2).reshape(EXPERTS, per_expert)

    def one_expert(operands):
        token_rows, w_gate, w_up, w_down = operands
        return expert_rows(expert_in[token_rows], w_gate, w_up, w_down)
    outputs = lax.map(one_expert, (tokens_of, gate_w, up_w, down_w))
    per_assign = jnp.zeros((flat_ids.shape[0], D), jnp.bfloat16).at[sort_order].set(outputs.reshape(-1, D))
    per_assign = per_assign.reshape(-1, 2, D)
    first_out = per_assign[:, 0].astype(jnp.float32)
    second = per_assign[:, 1].astype(jnp.float32)
    moe_out = (first_out * route_weight[:, 0:1] + second * route_weight[:, 1:2]).astype(jnp.bfloat16)
    return (mixed, moe_out)
```

```python
import functools

import jax
import jax.numpy as jnp
from jax import lax
from jax.experimental import pallas as pl
from jax.experimental.pallas import tpu as pltpu
from jax.sharding import PartitionSpec as P

MESH = pl.DeviceIdType.MESH
F32 = jnp.float32
BF16 = jnp.bfloat16
EPS = 1e-06

SIDE = 4
ORDER = (
    ((0, 0), (0, 1), (0, 3), (1, 0)),
    ((3, 3), (0, 2), (2, 0), (1, 2)),
    ((2, 1), (2, 3), (3, 2), (2, 2)),
    ((3, 0), (1, 1), (1, 3), (3, 1)),
)
OFFSETS = tuple(pair for chunk in ORDER for pair in chunk)
CHUNKS = len(ORDER)
PER_CHUNK = len(ORDER[0])
EP = len(OFFSETS)
TP = 8
GROUP_ROWS = 16
EXPERT_ROWS = 4
META = 128
TP_ORDER = (4, 5, 2, 3, 6, 7, 1)


def iota(shape, dim):
    return lax.broadcasted_iota(jnp.int32, shape, dim)


def hot(mask):
    return jnp.where(mask, 1.0, 0.0)


def dot(a, b, contract=((1,), (0,))):
    return lax.dot_general(a, b, (contract, ((), ())), preferred_element_type=F32)


def kernel(
    taps_ref,
    ggain_ref,
    mgain_ref,
    ids_ref,
    rw_ref,
    og_hbm,
    ig_hbm,
    ci_hbm,
    mixw_hbm,
    x_hbm,
    wg_hbm,
    wu_hbm,
    wd_hbm,
    mixed_hbm,
    moe_hbm,
    x_buf,
    xn_buf,
    og,
    ig,
    ci,
    edges,
    prod,
    normed,
    recvm,
    mixw,
    wg,
    wu,
    wd,
    perm,
    send1,
    recv1,
    send2,
    recv2,
    hid,
    send3,
    res,
    send4,
    ret,
    mixed_buf,
    moe_buf,
    load_sem,
    s1,
    r1,
    s2,
    r2,
    s3,
    r3,
    s4,
    r4,
    sm,
    rm,
    se,
    re,
    out_sem,
):
    ep = lax.axis_index("ep")
    tp = lax.axis_index("tp")
    z, x = ep // SIDE, ep % SIDE
    y, c = tp // 2, tp % 2
    width = x_buf.shape[1]
    tokens = x_buf.shape[0]

    def ep_peer(dz, dx):
        return (((z + dz) % SIDE) * SIDE + (x + dx) % SIDE, tp)

    def tp_peer(q, back=False):
        dy, dc = q // 2, q % 2
        dy = SIDE - dy if back else dy
        return (ep, ((y + dy) % SIDE) * 2 + (c + dc) % 2)

    def load(i, src, dst):
        cp = pltpu.make_async_copy(src, dst, load_sem.at[i])
        cp.start()
        return cp

    ld_x = load(0, x_hbm, x_buf)
    ld_ig = load(1, ig_hbm, ig)
    ld_ci = load(2, ci_hbm, ci)
    ld_og = load(3, og_hbm, og)
    ld_wg = load(4, wg_hbm.at[0], wg)
    ld_wu = load(5, wu_hbm.at[0], wu)
    ld_wd = load(6, wd_hbm.at[0], wd)
    ld_mw = load(7, mixw_hbm, mixw)

    barrier = pltpu.get_barrier_semaphore()
    for dz, dx in OFFSETS[1:]:
        pl.semaphore_signal(barrier, inc=1, device_id=ep_peer(dz, dx), device_id_type=MESH)
    for q in range(1, TP):
        pl.semaphore_signal(barrier, inc=1, device_id=tp_peer(q), device_id_type=MESH)

    sent = []

    def send(src, dst, ssem, rsem, device):
        cp = pltpu.make_async_remote_copy(
            src_ref=src, dst_ref=dst, send_sem=ssem, recv_sem=rsem, device_id=device, device_id_type=MESH
        )
        cp.start()
        sent.append(cp)
        return cp

    id0 = ids_ref[0:1, :]
    id1 = ids_ref[1:2, :]
    earlier = hot(iota((tokens, tokens), 0) < iota((tokens, tokens), 1)).astype(BF16)
    expert_of = iota((EP * TP, tokens), 0)
    hits0 = hot(expert_of == id0)
    hits1 = hot(expert_of == id1)
    before = dot((hits0 + hits1).astype(BF16), earlier)
    rank0 = jnp.sum(hits0 * before, axis=0, keepdims=True)
    rank1 = jnp.sum(hits1 * before, axis=0, keepdims=True)

    def base_slot(ids, rank):
        inner = ids & (TP - 1)
        dy = ((inner >> 1) - y) & (SIDE - 1)
        dc = ((inner & 1) + c) & 1
        return ((dy * 2 + dc) * GROUP_ROWS).astype(F32) + rank

    base0 = base_slot(id0, rank0)
    base1 = base_slot(id1, rank1)
    group = id0 >> 3
    place = (((group >> 2) - z) & 3) * SIDE + (((group & 3) - x) & 3)
    order = jnp.zeros_like(place)
    for k, (dz, dx) in enumerate(OFFSETS):
        order = jnp.where(place == dz * SIDE + dx, k, order)
    members = hot(iota((EP, tokens), 0) == order)
    group_rank = jnp.sum(members * dot(members.astype(BF16), earlier), axis=0, keepdims=True)
    slot = (order * GROUP_ROWS).astype(F32) + group_rank
    perm_f32 = hot(iota((tokens, tokens), 0).astype(F32) == slot)
    perm[...] = perm_f32.T.astype(BF16)
    forward = perm_f32.astype(BF16)
    w_hi = rw_ref[...].astype(BF16).astype(F32)
    w_lo = rw_ref[...] - w_hi
    meta_rows = jnp.concatenate(
        [base0, base1, w_hi[0:1], w_lo[0:1], w_hi[1:2], w_lo[1:2], jnp.zeros((META - 6, tokens), F32)], axis=0
    )
    meta = dot(forward, meta_rows.astype(BF16), ((1,), (1,))).astype(BF16)
    send1[:, width:] = meta
    recv1[0:GROUP_ROWS, width:] = meta[0:GROUP_ROWS]

    ld_x.wait()
    norm_rows = 32

    @pl.loop(0, tokens // norm_rows)
    def _(i):
        rows = pl.ds(pl.multiple_of(i * norm_rows, norm_rows), norm_rows)
        wide = x_buf[rows, :].astype(F32)
        scale = lax.rsqrt(jnp.mean(wide * wide, axis=-1, keepdims=True) + EPS)
        xn_buf[rows, :] = (wide * scale * mgain_ref[...]).astype(BF16)

    tile = 512

    @pl.loop(0, width // tile)
    def _(n):
        cols = pl.ds(pl.multiple_of(n * tile, tile), tile)
        moved = dot(forward, xn_buf[:, cols]).astype(BF16)
        send1[:, cols] = moved
        recv1[0:GROUP_ROWS, cols] = moved[0:GROUP_ROWS]

    ld_ig.wait()
    ld_ci.wait()
    pl.semaphore_wait(barrier, EP - 1 + TP - 1)

    length = ig.shape[0]
    after = (lax.rem(ep + 1, EP), tp)
    edge = [
        send(src.at[pl.ds(length - 16, 16)], edges.at[i], se.at[i], re.at[i], after)
        for i, src in enumerate((ig, ci))
    ]
    first = []
    for k in range(1, EP):
        rows = pl.ds(k * GROUP_ROWS, GROUP_ROWS)
        first.append(send(send1.at[rows], recv1.at[rows], s1.at[k], r1.at[k], ep_peer(*OFFSETS[k])))

    for cp in edge:
        cp.wait_recv()
    ld_og.wait()
    keep = jnp.where(ep > 0, 1.0, 0.0)
    prod[0:8, :] = edges[0].astype(F32)[8:16] * edges[1].astype(F32)[8:16] * keep
    step_rows = tokens

    @pl.loop(0, length // step_rows)
    def _(i):
        rows = pl.ds(pl.multiple_of(i * step_rows, step_rows), step_rows)
        prod[pl.ds(pl.multiple_of(i * step_rows + 8, 8), step_rows), :] = ig[rows, :].astype(F32) * ci[rows, :].astype(F32)

    same = hot((iota((META, META), 0) >> 6) == (iota((META, META), 1) >> 6))
    averager = (same * (1.0 / 64.0)).astype(BF16)

    @pl.loop(0, length // step_rows)
    def _(i):
        rows = pl.ds(pl.multiple_of(i * step_rows, step_rows), step_rows)
        block = prod[pl.ds(pl.multiple_of(i * step_rows, 8), step_rows + 8), :]
        convolved = (
            taps_ref[0:1, :] * pltpu.roll(block, 2, 0)[8:]
            + taps_ref[1:2, :] * pltpu.roll(block, 1, 0)[8:]
            + taps_ref[2:3, :] * block[8:]
        )
        gated = og[rows, :].astype(F32) * convolved
        square = gated * gated
        high = square.astype(BF16)
        low = (square - high.astype(F32)).astype(BF16)
        inv = lax.rsqrt(dot(high, averager) + dot(low, averager) + EPS)
        normed[rows, :] = (gated * inv * ggain_ref[...]).astype(BF16)

    own = pl.ds(pl.multiple_of(tp * tokens, tokens), tokens)
    recvm[tp] = normed[own, :]
    mix = []
    for q in TP_ORDER:
        peer = tp_peer(q)
        rows = pl.ds(pl.multiple_of(peer[1] * tokens, tokens), tokens)
        mix.append(send(normed.at[rows], recvm.at[tp], sm.at[q], rm.at[q], peer))

    chunk_in = PER_CHUNK * GROUP_ROWS
    chunk_out = TP * GROUP_ROWS

    def places(j):
        info = recv1[j * chunk_in : (j + 1) * chunk_in, width:].astype(F32)
        shift = ((iota((chunk_in, chunk_out), 0) >> 4) * EXPERT_ROWS).astype(F32)
        lane = iota((chunk_in, chunk_out), 1).astype(F32)
        return info, info[:, 0:1] + shift == lane, info[:, 1:2] + shift == lane

    second = []
    for j in range(CHUNKS):
        for k in range(max(1, j * PER_CHUNK), (j + 1) * PER_CHUNK):
            first[k - 1].wait_recv()
        _, at0, at1 = places(j)
        split = (hot(at0) + hot(at1)).T.astype(BF16)
        base = j * chunk_out

        @pl.loop(0, width // tile)
        def _(n):
            cols = pl.ds(pl.multiple_of(n * tile, tile), tile)
            moved = dot(split, recv1[j * chunk_in : (j + 1) * chunk_in, cols]).astype(BF16)
            send2[base : base + chunk_out, cols] = moved
            recv2[base : base + GROUP_ROWS, cols] = moved[0:GROUP_ROWS]

        arrivals = []
        for q in TP_ORDER:
            rows = pl.ds(base + q * GROUP_ROWS, GROUP_ROWS)
            arrivals.append(send(send2.at[rows], recv2.at[rows], s2.at[j, q], r2.at[j, q], tp_peer(q)))
        second.append(arrivals)

    ld_wg.wait()
    ld_wu.wait()
    ld_wd.wait()
    hidden_units = wg.shape[1]
    hid_tile = 256
    third = []
    for j in range(CHUNKS):
        for cp in second[j]:
            cp.wait_recv()
        base = j * chunk_out

        @pl.loop(0, hidden_units // hid_tile)
        def _(n):
            cols = pl.ds(pl.multiple_of(n * hid_tile, hid_tile), hid_tile)
            inputs = recv2[base : base + chunk_out, :]
            gate = dot(inputs, wg[:, cols])
            up = dot(inputs, wu[:, cols])
            hid[:, cols] = (gate / (1.0 + jnp.exp(-gate)) * up).astype(BF16)

        @pl.loop(0, width // tile)
        def _(n):
            cols = pl.ds(pl.multiple_of(n * tile, tile), tile)
            result = dot(hid[...], wd[:, cols]).astype(BF16)
            send3[base : base + chunk_out, cols] = result
            res[base : base + GROUP_ROWS, cols] = result[0:GROUP_ROWS]

        arrivals = []
        for q in TP_ORDER:
            rows = pl.ds(base + q * GROUP_ROWS, GROUP_ROWS)
            arrivals.append(send(send3.at[rows], res.at[rows], s3.at[j, q], r3.at[j, q], tp_peer(q, back=True)))
        third.append(arrivals)

    ld_mw.wait()
    for cp in mix:
        cp.wait_recv()

    @pl.loop(0, width // tile)
    def _(n):
        cols = pl.ds(pl.multiple_of(n * tile, tile), tile)
        total = jnp.zeros((tokens, tile), F32)
        for i in range(0, TP, 2):
            pair = jnp.concatenate([recvm[i], recvm[i + 1]], axis=1)
            total += dot(pair, mixw[i * META : (i + 2) * META, cols])
        mixed_buf[:, cols] = total.astype(BF16)

    out_mixed = pltpu.make_async_copy(mixed_buf, mixed_hbm, out_sem.at[0])
    out_mixed.start()

    last = []
    for j in range(CHUNKS):
        for cp in third[j]:
            cp.wait_recv()
        info, at0, at1 = places(j)
        high = (jnp.where(at0, info[:, 2:3], 0.0) + jnp.where(at1, info[:, 4:5], 0.0)).astype(BF16)
        low = (jnp.where(at0, info[:, 3:4], 0.0) + jnp.where(at1, info[:, 5:6], 0.0)).astype(BF16)
        base = j * chunk_in

        @pl.loop(0, width // tile)
        def _(n):
            cols = pl.ds(pl.multiple_of(n * tile, tile), tile)
            results = res[j * chunk_out : (j + 1) * chunk_out, cols]
            joined = (dot(high, results) + dot(low, results)).astype(BF16)
            send4[base : base + chunk_in, cols] = joined
            if j == 0:
                ret[0:GROUP_ROWS, cols] = joined[0:GROUP_ROWS]

        for k in range(max(1, j * PER_CHUNK), (j + 1) * PER_CHUNK):
            dz, dx = OFFSETS[k]
            rows = pl.ds(k * GROUP_ROWS, GROUP_ROWS)
            last.append(send(send4.at[rows], ret.at[rows], s4.at[k], r4.at[k], ep_peer(SIDE - dz, SIDE - dx)))

    for cp in last:
        cp.wait_recv()

    @pl.loop(0, width // tile)
    def _(n):
        cols = pl.ds(pl.multiple_of(n * tile, tile), tile)
        moe_buf[:, cols] = dot(perm[...], ret[:, cols]).astype(BF16)

    out_moe = pltpu.make_async_copy(moe_buf, moe_hbm, out_sem.at[1])
    out_moe.start()
    for cp in sent:
        cp.wait_send()
    out_mixed.wait()
    out_moe.wait()


def shards(
    out_gate, in_gate, conv_input, conv_taps, group_gain, mix_out_w, moe_in, moe_gain, route_ids, route_weight,
    gate_w, up_w, down_w,
):
    rows, channels = in_gate.shape
    tokens, width = moe_in.shape
    hidden = gate_w.shape[2]
    vmem = pl.BlockSpec(memory_space=pltpu.VMEM)
    hbm = pl.BlockSpec(memory_space=pl.ANY)
    dma = pltpu.SemaphoreType.DMA
    out = jax.ShapeDtypeStruct((tokens, width), BF16)
    V = pltpu.VMEM
    slots = 2 * tokens
    return pl.pallas_call(
        kernel,
        out_shape=(out, out),
        in_specs=[vmem] * 5 + [hbm] * 8,
        out_specs=(hbm, hbm),
        scratch_shapes=[
            V((tokens, width), BF16),
            V((tokens, width), BF16),
            V((rows, channels), BF16),
            V((rows, channels), BF16),
            V((rows, channels), BF16),
            V((2, 16, channels), BF16),
            V((rows + 8, channels), F32),
            V((rows, channels), BF16),
            V((TP, tokens, channels), BF16),
            V(mix_out_w.shape, BF16),
            V((width, hidden), BF16),
            V((width, hidden), BF16),
            V((hidden, width), BF16),
            V((tokens, tokens), BF16),
            V((tokens, width + META), BF16),
            V((tokens, width + META), BF16),
            V((slots, width), BF16),
            V((slots, width), BF16),
            V((TP * GROUP_ROWS, hidden), BF16),
            V((slots, width), BF16),
            V((slots, width), BF16),
            V((tokens, width), BF16),
            V((tokens, width), BF16),
            V((tokens, width), BF16),
            V((tokens, width), BF16),
            dma((8,)),
            dma((EP,)), dma((EP,)),
            dma((CHUNKS, TP)), dma((CHUNKS, TP)),
            dma((CHUNKS, TP)), dma((CHUNKS, TP)),
            dma((EP,)), dma((EP,)),
            dma((TP,)), dma((TP,)),
            dma((2,)), dma((2,)),
            dma((2,)),
        ],
        compiler_params=pltpu.CompilerParams(
            collective_id=0, has_side_effects=True, vmem_limit_bytes=60 * 1024 * 1024
        ),
    )(
        conv_taps, group_gain.reshape(1, -1), moe_gain.reshape(1, -1), route_ids.T, route_weight.T,
        out_gate, in_gate, conv_input, mix_out_w, moe_in, gate_w, up_w, down_w,
    )


def solution(mesh):
    both = ("ep", "tp")
    in_specs = (
        P("ep", "tp"), P("ep", "tp"), P("ep", "tp"), P(None, "tp"), P("tp"), P(),
        P(both, None), P(), P(both, None), P(both, None),
        P(both, None, None), P(both, None, None), P(both, None, None),
    )
    return jax.shard_map(
        shards, mesh=mesh, in_specs=in_specs, out_specs=(P(both, None), P(both, None)), check_vma=False
    )
```

```python
import functools

import jax
import jax.numpy as jnp
from jax import lax
from jax.experimental import pallas as pl
from jax.experimental.pallas import tpu as pltpu
from jax.sharding import PartitionSpec as P

MESH = pl.DeviceIdType.MESH
F32 = jnp.float32
BF16 = jnp.bfloat16
EPS = 1e-06

SIDE = 4
ORDER = (
    ((1, 2), (2, 1), (0, 2), (2, 0)),
    ((2, 2), (2, 3), (3, 2), (1, 1)),
    ((3, 0), (1, 3), (3, 1), (3, 3)),
    ((0, 0), (0, 1), (1, 0), (0, 3)),
)
OFFSETS = tuple(pair for chunk in ORDER for pair in chunk)
CHUNKS = len(ORDER)
SELF = OFFSETS.index((0, 0))
SPLIT_ORDER = (3, 0, 1, 2)
PER_CHUNK = len(ORDER[0])
EP = len(OFFSETS)
TP = 8
GROUP_ROWS = 16
EXPERT_ROWS = 4
META = 128
TP_ORDER = (4, 5, 2, 3, 6, 7, 1)
MIX_EARLY = (4, 5, 1)
MIX_LATE = (2, 3, 6, 7)


def chunk_peers(j):
    return [k for k in range(j * PER_CHUNK, (j + 1) * PER_CHUNK) if k != SELF]


def iota(shape, dim):
    return lax.broadcasted_iota(jnp.int32, shape, dim)


def hot(mask):
    return jnp.where(mask, 1.0, 0.0)


def dot(a, b, contract=((1,), (0,))):
    return lax.dot_general(a, b, (contract, ((), ())), preferred_element_type=F32)


def kernel(
    taps_hbm,
    ggain_hbm,
    mgain_hbm,
    ids_hbm,
    rw_hbm,
    og_hbm,
    ig_hbm,
    ci_hbm,
    mixw_hbm,
    x_hbm,
    wg_hbm,
    wu_hbm,
    wd_hbm,
    mixed_hbm,
    ret_hbm,
    perm_hbm,
    taps_ref,
    ggain_ref,
    mgain_ref,
    ids_ref,
    rw_ref,
    x_buf,
    xn_buf,
    og,
    ig,
    ci,
    edges,
    prod,
    normed,
    recvm,
    mixw,
    wg,
    wu,
    wd,
    perm,
    send1,
    recv1,
    send2,
    recv2,
    hid,
    send3,
    res,
    send4,
    mixed_sum,
    mixed_buf,
    load_sem,
    s1,
    r1,
    s2,
    r2,
    s3,
    r3,
    s4,
    r4,
    sm,
    rm,
    se,
    re,
    out_sem,
    mix_sem,
):
    ep = lax.axis_index("ep")
    tp = lax.axis_index("tp")
    z, x = ep // SIDE, ep % SIDE
    y, c = tp // 2, tp % 2
    width = x_buf.shape[1]
    tokens = x_buf.shape[0]

    def ep_peer(dz, dx):
        return (((z + dz) % SIDE) * SIDE + (x + dx) % SIDE, tp)

    def tp_peer(q, back=False):
        dy, dc = q // 2, q % 2
        dy = SIDE - dy if back else dy
        return (ep, ((y + dy) % SIDE) * 2 + (c + dc) % 2)

    def load(i, src, dst):
        cp = pltpu.make_async_copy(src, dst, load_sem.at[i])
        cp.start()
        return cp

    ld_ids = load(8, ids_hbm, ids_ref)
    ld_rw = load(9, rw_hbm, rw_ref)
    ld_x = load(0, x_hbm, x_buf)
    ld_mgain = load(10, mgain_hbm, mgain_ref)
    ld_ig = load(1, ig_hbm, ig)
    ld_ci = load(2, ci_hbm, ci)
    ld_og = load(3, og_hbm, og)
    ld_taps = load(11, taps_hbm, taps_ref)
    ld_ggain = load(12, ggain_hbm, ggain_ref)
    ld_wg = load(4, wg_hbm.at[0], wg)
    ld_wu = load(5, wu_hbm.at[0], wu)
    ld_wd = load(6, wd_hbm.at[0], wd)
    ld_mw = load(7, mixw_hbm, mixw)

    barrier = pltpu.get_barrier_semaphore()
    for k in range(EP):
        if k == SELF:
            continue
        dz, dx = OFFSETS[k]
        pl.semaphore_signal(barrier, inc=1, device_id=ep_peer(dz, dx), device_id_type=MESH)
    for q in range(1, TP):
        pl.semaphore_signal(barrier, inc=1, device_id=tp_peer(q), device_id_type=MESH)

    sent = []

    def send(src, dst, ssem, rsem, device):
        cp = pltpu.make_async_remote_copy(
            src_ref=src, dst_ref=dst, send_sem=ssem, recv_sem=rsem, device_id=device, device_id_type=MESH
        )
        cp.start()
        sent.append(cp)
        return cp

    ld_ids.wait()
    ld_rw.wait()
    id0 = ids_ref[0:1, :]
    id1 = ids_ref[1:2, :]
    earlier = hot(iota((tokens, tokens), 0) < iota((tokens, tokens), 1)).astype(BF16)
    expert_of = iota((EP * TP, tokens), 0)
    hits0 = hot(expert_of == id0)
    hits1 = hot(expert_of == id1)
    before = dot((hits0 + hits1).astype(BF16), earlier)
    rank0 = jnp.sum(hits0 * before, axis=0, keepdims=True)
    rank1 = jnp.sum(hits1 * before, axis=0, keepdims=True)

    def base_slot(ids, rank):
        inner = ids & (TP - 1)
        dy = ((inner >> 1) - y) & (SIDE - 1)
        dc = ((inner & 1) + c) & 1
        return ((dy * 2 + dc) * GROUP_ROWS).astype(F32) + rank

    base0 = base_slot(id0, rank0)
    base1 = base_slot(id1, rank1)
    group = id0 >> 3
    place = (((group >> 2) - z) & 3) * SIDE + (((group & 3) - x) & 3)
    order = jnp.zeros_like(place)
    for k, (dz, dx) in enumerate(OFFSETS):
        order = jnp.where(place == dz * SIDE + dx, k, order)
    members = hot(iota((EP, tokens), 0) == order)
    group_rank = jnp.sum(members * dot(members.astype(BF16), earlier), axis=0, keepdims=True)
    slot = (order * GROUP_ROWS).astype(F32) + group_rank
    perm_f32 = hot(iota((tokens, tokens), 0).astype(F32) == slot)
    perm[...] = perm_f32.T.astype(BF16)
    out_perm = pltpu.make_async_copy(perm, perm_hbm, out_sem.at[1])
    out_perm.start()
    forward = perm_f32.astype(BF16)
    w_hi = rw_ref[...].astype(BF16).astype(F32)
    w_lo = rw_ref[...] - w_hi
    meta_rows = jnp.concatenate(
        [base0, base1, w_hi[0:1], w_lo[0:1], w_hi[1:2], w_lo[1:2], jnp.zeros((META - 6, tokens), F32)], axis=0
    )
    meta = dot(forward, meta_rows.astype(BF16), ((1,), (1,))).astype(BF16)
    send1[:, width:] = meta
    mine = slice(SELF * GROUP_ROWS, (SELF + 1) * GROUP_ROWS)
    recv1[mine, width:] = meta[mine]

    ld_x.wait()
    ld_mgain.wait()
    norm_rows = 32

    @pl.loop(0, tokens // norm_rows)
    def _(i):
        rows = pl.ds(pl.multiple_of(i * norm_rows, norm_rows), norm_rows)
        wide = x_buf[rows, :].astype(F32)
        scale = lax.rsqrt(jnp.mean(wide * wide, axis=-1, keepdims=True) + EPS)
        xn_buf[rows, :] = (wide * scale * mgain_ref[...]).astype(BF16)

    tile = 512

    @pl.loop(0, width // tile)
    def _(n):
        cols = pl.ds(pl.multiple_of(n * tile, tile), tile)
        moved = dot(forward, xn_buf[:, cols]).astype(BF16)
        send1[:, cols] = moved
        recv1[mine, cols] = moved[mine]

    ld_ig.wait()
    ld_ci.wait()
    pl.semaphore_wait(barrier, EP - 1 + TP - 1)

    length = ig.shape[0]
    after = (lax.rem(ep + 1, EP), tp)
    edge = [
        send(src.at[pl.ds(length - 16, 16)], edges.at[i], se.at[i], re.at[i], after)
        for i, src in enumerate((ig, ci))
    ]
    first = {}
    for j in SPLIT_ORDER:
        for k in chunk_peers(j):
            rows = pl.ds(k * GROUP_ROWS, GROUP_ROWS)
            first[k] = send(send1.at[rows], recv1.at[rows], s1.at[k], r1.at[k], ep_peer(*OFFSETS[k]))

    ld_og.wait()
    ld_taps.wait()
    ld_ggain.wait()

    @pl.loop(0, length // tokens)
    def _(i):
        rows = pl.ds(pl.multiple_of(i * tokens, tokens), tokens)
        prod[pl.ds(pl.multiple_of(i * tokens + 8, 8), tokens), :] = ig[rows, :].astype(F32) * ci[rows, :].astype(F32)

    same = hot((iota((META, META), 0) >> 6) == (iota((META, META), 1) >> 6))
    averager = (same * (1.0 / 64.0)).astype(BF16)

    def convolve(i):
        rows = pl.ds(pl.multiple_of(i * tokens, tokens), tokens)
        block = prod[pl.ds(pl.multiple_of(i * tokens, 8), tokens + 8), :]
        convolved = (
            taps_ref[0:1, :] * pltpu.roll(block, 2, 0)[8:]
            + taps_ref[1:2, :] * pltpu.roll(block, 1, 0)[8:]
            + taps_ref[2:3, :] * block[8:]
        )
        gated = og[rows, :].astype(F32) * convolved
        square = gated * gated
        high = square.astype(BF16)
        low = (square - high.astype(F32)).astype(BF16)
        inv = lax.rsqrt(dot(high, averager) + dot(low, averager) + EPS)
        normed[rows, :] = (gated * inv * ggain_ref[...]).astype(BF16)

    pl.loop(1, length // tokens)(convolve)
    for cp in edge:
        cp.wait_recv()
    keep = jnp.where(ep > 0, 1.0, 0.0)
    prod[0:8, :] = edges[0].astype(F32)[8:16] * edges[1].astype(F32)[8:16] * keep
    convolve(0)

    recvm[tp] = normed[pl.ds(pl.multiple_of(tp * tokens, tokens), tokens), :]

    def send_mixer(q):
        peer = tp_peer(q)
        rows = pl.ds(pl.multiple_of(peer[1] * tokens, tokens), tokens)
        return send(normed.at[rows], recvm.at[tp], sm.at[q], rm.at[q], peer)

    mix_early = [send_mixer(q) for q in MIX_EARLY]

    chunk_in = PER_CHUNK * GROUP_ROWS
    chunk_out = TP * GROUP_ROWS

    def places(j):
        info = recv1[j * chunk_in : (j + 1) * chunk_in, width:].astype(F32)
        shift = ((iota((chunk_in, chunk_out), 0) >> 4) * EXPERT_ROWS).astype(F32)
        lane = iota((chunk_in, chunk_out), 1).astype(F32)
        return info, info[:, 0:1] + shift == lane, info[:, 1:2] + shift == lane

    second = {}
    for j in SPLIT_ORDER:
        for k in chunk_peers(j):
            first[k].wait_recv()
        _, at0, at1 = places(j)
        split = (hot(at0) + hot(at1)).T.astype(BF16)
        base = j * chunk_out

        @pl.loop(0, width // tile)
        def _(n):
            cols = pl.ds(pl.multiple_of(n * tile, tile), tile)
            moved = dot(split, recv1[j * chunk_in : (j + 1) * chunk_in, cols]).astype(BF16)
            send2[base : base + chunk_out, cols] = moved
            recv2[base : base + GROUP_ROWS, cols] = moved[0:GROUP_ROWS]

        arrivals = []
        for q in TP_ORDER:
            rows = pl.ds(base + q * GROUP_ROWS, GROUP_ROWS)
            arrivals.append(send(send2.at[rows], recv2.at[rows], s2.at[j, q], r2.at[j, q], tp_peer(q)))
        second[j] = arrivals

    ld_wg.wait()
    ld_wu.wait()
    ld_wd.wait()
    hidden_units = wg.shape[1]
    hid_tile = 256
    third = []
    for j in range(CHUNKS):
        for cp in second[j]:
            cp.wait_recv()
        base = j * chunk_out

        @pl.loop(0, hidden_units // hid_tile)
        def _(n):
            cols = pl.ds(pl.multiple_of(n * hid_tile, hid_tile), hid_tile)
            inputs = recv2[base : base + chunk_out, :]
            gate = dot(inputs, wg[:, cols])
            up = dot(inputs, wu[:, cols])
            hid[:, cols] = (gate / (1.0 + jnp.exp(-gate)) * up).astype(BF16)

        @pl.loop(0, width // tile)
        def _(n):
            cols = pl.ds(pl.multiple_of(n * tile, tile), tile)
            result = dot(hid[...], wd[:, cols]).astype(BF16)
            send3[base : base + chunk_out, cols] = result
            res[base : base + GROUP_ROWS, cols] = result[0:GROUP_ROWS]

        arrivals = []
        for q in TP_ORDER:
            rows = pl.ds(base + q * GROUP_ROWS, GROUP_ROWS)
            arrivals.append(send(send3.at[rows], res.at[rows], s3.at[j, q], r3.at[j, q], tp_peer(q, back=True)))
        third.append(arrivals)

    mix_late = [send_mixer(q) for q in MIX_LATE]

    def chip_part(dy, cols):
        chip = (y + dy) % SIDE
        pair = jnp.concatenate([recvm[chip * 2], recvm[chip * 2 + 1]], axis=1)
        weights = mixw[pl.ds(pl.multiple_of(chip * (2 * META), 2 * META), 2 * META), cols]
        return dot(pair, weights)

    ld_mw.wait()
    for cp in mix_early:
        cp.wait_recv()

    @pl.loop(0, width // tile)
    def _(n):
        cols = pl.ds(pl.multiple_of(n * tile, tile), tile)
        mixed_sum[:, cols] = chip_part(0, cols) + chip_part(2, cols)

    last = []
    for j in range(CHUNKS):
        for cp in third[j]:
            cp.wait_recv()
        info, at0, at1 = places(j)
        high = (jnp.where(at0, info[:, 2:3], 0.0) + jnp.where(at1, info[:, 4:5], 0.0)).astype(BF16)
        low = (jnp.where(at0, info[:, 3:4], 0.0) + jnp.where(at1, info[:, 5:6], 0.0)).astype(BF16)
        base = j * chunk_in

        @pl.loop(0, width // tile)
        def _(n):
            cols = pl.ds(pl.multiple_of(n * tile, tile), tile)
            results = res[j * chunk_out : (j + 1) * chunk_out, cols]
            joined = (dot(high, results) + dot(low, results)).astype(BF16)
            send4[base : base + chunk_in, cols] = joined

        for k in chunk_peers(j):
            dz, dx = OFFSETS[k]
            rows = pl.ds(k * GROUP_ROWS, GROUP_ROWS)
            last.append(send(send4.at[rows], ret_hbm.at[rows], s4.at[k], r4.at[k], ep_peer(SIDE - dz, SIDE - dx)))

    home = pl.ds(SELF * GROUP_ROWS, GROUP_ROWS)
    own = pltpu.make_async_copy(send4.at[home], ret_hbm.at[home], out_sem.at[0])
    own.start()

    for cp in mix_late:
        cp.wait_recv()
    outs = []
    for n in range(width // tile):
        cols = slice(n * tile, (n + 1) * tile)
        mixed_buf[:, cols] = (mixed_sum[:, cols] + chip_part(1, cols) + chip_part(3, cols)).astype(BF16)
        cp = pltpu.make_async_copy(mixed_buf.at[:, cols], mixed_hbm.at[:, cols], mix_sem.at[n])
        cp.start()
        outs.append(cp)

    for cp in sent:
        cp.wait_send()
    for cp in outs:
        cp.wait()
    own.wait()
    out_perm.wait()
    for cp in last:
        cp.wait_recv()


def finish(perm_hbm, ret_hbm, mixed_hbm, out_mixed, out_moe, perm, ret, mixed, moe, in_sem, out_sem):
    tokens, width = ret.shape
    steps = in_sem.shape[1]
    tile = width // steps
    ld_perm = pltpu.make_async_copy(perm_hbm, perm, in_sem.at[2, 0])
    ld_perm.start()
    cols = [slice(n * tile, (n + 1) * tile) for n in range(steps)]

    def copies(src, dst, sem):
        return [pltpu.make_async_copy(src.at[:, cols[n]], dst.at[:, cols[n]], sem.at[n]) for n in range(steps)]

    rows_in = copies(ret_hbm, ret, in_sem.at[0])
    mixed_in = copies(mixed_hbm, mixed, in_sem.at[1])
    moe_out = copies(moe, out_moe, out_sem.at[0])
    mixed_out = copies(mixed, out_mixed, out_sem.at[1])
    for cp in rows_in + mixed_in:
        cp.start()
    ld_perm.wait()
    for n in range(steps):
        rows_in[n].wait()
        moe[:, cols[n]] = dot(perm[...], ret[:, cols[n]]).astype(BF16)
        moe_out[n].start()
        mixed_in[n].wait()
        mixed_out[n].start()
    for cp in moe_out + mixed_out:
        cp.wait()


def shards(
    out_gate, in_gate, conv_input, conv_taps, group_gain, mix_out_w, moe_in, moe_gain, route_ids, route_weight,
    gate_w, up_w, down_w,
):
    rows, channels = in_gate.shape
    tokens, width = moe_in.shape
    hidden = gate_w.shape[2]
    hbm = pl.BlockSpec(memory_space=pl.ANY)
    dma = pltpu.SemaphoreType.DMA
    out = jax.ShapeDtypeStruct((tokens, width), BF16)
    V = pltpu.VMEM
    slots = 2 * tokens
    square = jax.ShapeDtypeStruct((tokens, tokens), BF16)
    mixed, returned, perm = pl.pallas_call(
        kernel,
        out_shape=(out, out, square),
        in_specs=[hbm] * 13,
        out_specs=(hbm, hbm, hbm),
        scratch_shapes=[
            V(conv_taps.shape, F32),
            V((1, channels), F32),
            V((1, width), F32),
            V((2, tokens), jnp.int32),
            V((2, tokens), F32),
            V((tokens, width), BF16),
            V((tokens, width), BF16),
            V((rows, channels), BF16),
            V((rows, channels), BF16),
            V((rows, channels), BF16),
            V((2, 16, channels), BF16),
            V((rows + 8, channels), F32),
            V((rows, channels), BF16),
            V((TP, tokens, channels), BF16),
            V(mix_out_w.shape, BF16),
            V((width, hidden), BF16),
            V((width, hidden), BF16),
            V((hidden, width), BF16),
            V((tokens, tokens), BF16),
            V((tokens, width + META), BF16),
            V((tokens, width + META), BF16),
            V((slots, width), BF16),
            V((slots, width), BF16),
            V((TP * GROUP_ROWS, hidden), BF16),
            V((slots, width), BF16),
            V((slots, width), BF16),
            V((tokens, width), BF16),
            V((tokens, width), F32),
            V((tokens, width), BF16),
            dma((13,)),
            dma((EP,)), dma((EP,)),
            dma((CHUNKS, TP)), dma((CHUNKS, TP)),
            dma((CHUNKS, TP)), dma((CHUNKS, TP)),
            dma((EP,)), dma((EP,)),
            dma((TP,)), dma((TP,)),
            dma((2,)), dma((2,)),
            dma((2,)),
            dma((4,)),
        ],
        compiler_params=pltpu.CompilerParams(
            collective_id=0, has_side_effects=True, vmem_limit_bytes=60 * 1024 * 1024
        ),
    )(
        conv_taps, group_gain.reshape(1, -1), moe_gain.reshape(1, -1), route_ids.T, route_weight.T,
        out_gate, in_gate, conv_input, mix_out_w, moe_in, gate_w, up_w, down_w,
    )
    steps = 4
    return pl.pallas_call(
        finish,
        out_shape=(out, out),
        in_specs=[hbm] * 3,
        out_specs=(hbm, hbm),
        scratch_shapes=[
            V((tokens, tokens), BF16),
            V((tokens, width), BF16),
            V((tokens, width), BF16),
            V((tokens, width), BF16),
            dma((3, steps)),
            dma((2, steps)),
        ],
    )(perm, returned, mixed)


def solution(mesh):
    both = ("ep", "tp")
    in_specs = (
        P("ep", "tp"), P("ep", "tp"), P("ep", "tp"), P(None, "tp"), P("tp"), P(),
        P(both, None), P(), P(both, None), P(both, None),
        P(both, None, None), P(both, None, None), P(both, None, None),
    )
    return jax.shard_map(
        shards, mesh=mesh, in_specs=in_specs, out_specs=(P(both, None), P(both, None)), check_vma=False
    )
```

```python
import functools

import jax
import jax.numpy as jnp
from jax import lax
from jax.experimental import pallas as pl
from jax.experimental.pallas import tpu as pltpu
from jax.sharding import PartitionSpec as P

MESH = pl.DeviceIdType.MESH
F32 = jnp.float32
BF16 = jnp.bfloat16
EPS = 1e-06

SIDE = 4
ORDER = (
    ((1, 2), (2, 1), (0, 2), (2, 0)),
    ((2, 2), (2, 3), (3, 2), (1, 1)),
    ((3, 0), (1, 3), (3, 1), (3, 3)),
    ((0, 0), (0, 1), (1, 0), (0, 3)),
)
OFFSETS = tuple(pair for chunk in ORDER for pair in chunk)
CHUNKS = len(ORDER)
SELF = OFFSETS.index((0, 0))
SPLIT_ORDER = (3, 0, 1, 2)
PER_CHUNK = len(ORDER[0])
EP = len(OFFSETS)
TP = 8
GROUP_ROWS = 16
EXPERT_ROWS = 4
META = 128
GROUP_CH = 64
TP_ORDER = (4, 5, 2, 3, 6, 7, 1)
MIX_GROUPS = ((4, 5), (2, 3, 1), (6, 7))
NEAR = CHUNKS - 1
EDGE = 16


def chunk_peers(j):
    return [k for k in range(j * PER_CHUNK, (j + 1) * PER_CHUNK) if k != SELF]


def iota(shape, dim):
    return lax.broadcasted_iota(jnp.int32, shape, dim)


def hot(mask):
    return jnp.where(mask, 1.0, 0.0)


def dot(a, b, contract=((1,), (0,))):
    return lax.dot_general(a, b, (contract, ((), ())), preferred_element_type=F32)


def kernel(
    taps_hbm, ggain_hbm, mgain_hbm, ids_hbm, rw_hbm, og_hbm, ig_hbm, ci_hbm, mixw_hbm, x_hbm, wg_hbm, wu_hbm, wd_hbm,
    mixed, ret, perm,
    taps_ref, ggain_ref, mgain_ref, ids_ref, rw_ref,
    x_buf, xn_buf, og, ig, ci, normed, recvm, mixw, wg, wu, wd,
    send1, recv1, send2, recv2, hid, send3, res, send4, mixed_sum,
    load_sem, sent_sem, r1, r2, r3, r4, rm, re,
):
    ep = lax.axis_index("ep")
    tp = lax.axis_index("tp")
    z, x = ep // SIDE, ep % SIDE
    y, c = tp // 2, tp % 2
    tokens, width = x_buf.shape
    length = og.shape[0]

    def ep_peer(dz, dx):
        return (((z + dz) % SIDE) * SIDE + (x + dx) % SIDE, tp)

    def tp_peer(q, back=False):
        dy, dc = q // 2, q % 2
        dy = SIDE - dy if back else dy
        return (ep, ((y + dy) % SIDE) * 2 + (c + dc) % 2)

    def load(i, src, dst):
        cp = pltpu.make_async_copy(src, dst, load_sem.at[i])
        cp.start()
        return cp

    ld_ids = load(8, ids_hbm, ids_ref)
    ld_rw = load(9, rw_hbm, rw_ref)
    inner = pl.ds(EDGE, length)
    ld_ig = load(1, ig_hbm, ig.at[inner])
    ld_ci = load(2, ci_hbm, ci.at[inner])
    ld_og = load(3, og_hbm, og)
    ld_taps = load(11, taps_hbm, taps_ref)
    ld_ggain = load(12, ggain_hbm, ggain_ref)
    ld_x = load(0, x_hbm, x_buf)
    ld_mgain = load(10, mgain_hbm, mgain_ref)

    barrier = pltpu.get_barrier_semaphore()
    for k in range(EP):
        if k == SELF:
            continue
        dz, dx = OFFSETS[k]
        pl.semaphore_signal(barrier, inc=1, device_id=ep_peer(dz, dx), device_id_type=MESH)
    for q in range(1, TP):
        pl.semaphore_signal(barrier, inc=1, device_id=tp_peer(q), device_id_type=MESH)

    ld_wg = load(4, wg_hbm.at[0], wg)
    ld_wu = load(5, wu_hbm.at[0], wu)
    ld_wd = load(6, wd_hbm.at[0], wd)
    ld_mw = load(7, mixw_hbm, mixw)

    def send(src, dst, ssem, rsem, device):
        pltpu.make_async_remote_copy(
            src_ref=src, dst_ref=dst, send_sem=ssem, recv_sem=rsem, device_id=device, device_id_type=MESH
        ).start()

    def arrived(ref, sem):
        pltpu.make_async_remote_copy(
            src_ref=ref, dst_ref=ref, send_sem=sem, recv_sem=sem, device_id=tp_peer(1), device_id_type=MESH
        ).wait_recv()

    def departed(ref, sem):
        pltpu.make_async_remote_copy(
            src_ref=ref, dst_ref=ref, send_sem=sem, recv_sem=sem, device_id=tp_peer(1), device_id_type=MESH
        ).wait_send()

    ld_ids.wait()
    ld_rw.wait()
    id0 = ids_ref[0:1, :]
    id1 = ids_ref[1:2, :]
    earlier = hot(iota((tokens, tokens), 0) < iota((tokens, tokens), 1)).astype(BF16)
    expert_of = iota((EP * TP, tokens), 0)
    hits0 = hot(expert_of == id0)
    hits1 = hot(expert_of == id1)
    before = dot((hits0 + hits1).astype(BF16), earlier)
    rank0 = jnp.sum(hits0 * before, axis=0, keepdims=True)
    rank1 = jnp.sum(hits1 * before, axis=0, keepdims=True)

    def base_slot(ids, rank):
        inner = ids & (TP - 1)
        dy = ((inner >> 1) - y) & (SIDE - 1)
        dc = ((inner & 1) + c) & 1
        return ((dy * 2 + dc) * GROUP_ROWS).astype(F32) + rank

    base0 = base_slot(id0, rank0)
    base1 = base_slot(id1, rank1)
    group = id0 >> 3
    place = (((group >> 2) - z) & 3) * SIDE + (((group & 3) - x) & 3)
    order = jnp.zeros_like(place)
    for k, (dz, dx) in enumerate(OFFSETS):
        order = jnp.where(place == dz * SIDE + dx, k, order)
    members = hot(iota((EP, tokens), 0) == order)
    group_rank = jnp.sum(members * dot(members.astype(BF16), earlier), axis=0, keepdims=True)
    slot = (order * GROUP_ROWS).astype(F32) + group_rank
    perm_f32 = hot(iota((tokens, tokens), 0).astype(F32) == slot)
    forward = perm_f32.astype(BF16)
    w_hi = rw_ref[...].astype(BF16).astype(F32)
    w_lo = rw_ref[...] - w_hi
    meta_rows = jnp.concatenate(
        [base0, base1, w_hi[0:1], w_lo[0:1], w_hi[1:2], w_lo[1:2], jnp.zeros((META - 6, tokens), F32)], axis=0
    )
    meta = dot(forward, meta_rows.astype(BF16), ((1,), (1,))).astype(BF16)
    mine = slice(SELF * GROUP_ROWS, (SELF + 1) * GROUP_ROWS)
    send1[:, 0:META] = meta
    recv1[mine, 0:META] = meta[mine]

    ld_ig.wait()
    ld_ci.wait()
    pl.semaphore_wait(barrier, EP - 1 + TP - 1)
    after = (lax.rem(ep + 1, EP), tp)
    for ref in (ig, ci):
        send(ref.at[pl.ds(length, EDGE)], ref.at[pl.ds(0, EDGE)], sent_sem.at[5], re.at[0], after)

    ld_og.wait()
    ld_taps.wait()
    ld_ggain.wait()
    same = hot((iota((META, META), 0) >> 6) == (iota((META, META), 1) >> 6))
    averager = (same * (1.0 / GROUP_CH)).astype(BF16)

    def convolve(i):
        rows = pl.ds(pl.multiple_of(i * tokens, tokens), tokens)
        wide = pl.ds(pl.multiple_of(i * tokens, EDGE), tokens + EDGE)
        block = ig[wide, :].astype(F32) * ci[wide, :].astype(F32)
        keep = jnp.where(ep * TP + i > 0, 1.0, 0.0)
        block = jnp.concatenate([block[0:EDGE] * keep, block[EDGE:]], axis=0)
        convolved = (
            taps_ref[0:1, :] * pltpu.roll(block, 2, 0)[EDGE:]
            + taps_ref[1:2, :] * pltpu.roll(block, 1, 0)[EDGE:]
            + taps_ref[2:3, :] * block[EDGE:]
        )
        gated = og[rows, :].astype(F32) * convolved
        square = gated * gated
        high = square.astype(BF16)
        low = (square - high.astype(F32)).astype(BF16)
        inv = lax.rsqrt(dot(high, averager) + dot(low, averager) + EPS)
        normed[rows, :] = (gated * inv * ggain_ref[...]).astype(BF16)

    def convolve_chip(chip):
        convolve(chip * 2)
        convolve(chip * 2 + 1)

    def send_mixer(group):
        for q in MIX_GROUPS[group]:
            peer = tp_peer(q)
            rows = pl.ds(pl.multiple_of(peer[1] * tokens, tokens), tokens)
            send(normed.at[rows], recvm.at[tp], sent_sem.at[4], rm.at[group], peer)

    @pl.when(y == 2)
    def _():
        arrived(ig.at[pl.ds(0, 2 * EDGE)], re.at[0])

    convolve_chip((y + 2) % SIDE)
    send_mixer(0)

    ld_x.wait()
    ld_mgain.wait()
    wide_in = x_buf[...].astype(F32)
    scale = lax.rsqrt(jnp.mean(wide_in * wide_in, axis=-1, keepdims=True) + EPS)
    tile = 512
    tiles = [slice(n * tile, (n + 1) * tile) for n in range(width // tile)]
    half = len(tiles) // 2
    near = slice(NEAR * PER_CHUNK * GROUP_ROWS, tokens)
    halves = (pl.ds(0, META + width // 2), pl.ds(META + width // 2, width // 2))

    def shifted(cols):
        return slice(cols.start + META, cols.stop + META)

    def send_first(j, cols, sem):
        for k in chunk_peers(j):
            rows = pl.ds(k * GROUP_ROWS, GROUP_ROWS)
            send(send1.at[rows, cols], recv1.at[rows, cols], sent_sem.at[0], sem, ep_peer(*OFFSETS[k]))

    for n, cols in enumerate(tiles):
        tile_in = (x_buf[:, cols].astype(F32) * scale * mgain_ref[:, cols]).astype(BF16)
        xn_buf[:, cols] = tile_in
        moved = dot(forward[near], tile_in).astype(BF16)
        send1[near, shifted(cols)] = moved
        recv1[mine, shifted(cols)] = moved[mine.start - near.start : mine.stop - near.start]
        if n == half - 1:
            send_first(NEAR, halves[0], r1.at[NEAR])
    send_first(NEAR, halves[1], r1.at[CHUNKS])
    far = slice(0, near.start)
    for cols in tiles:
        send1[far, shifted(cols)] = dot(forward[far], xn_buf[:, cols]).astype(BF16)
    row = pl.ds(0, META + width)
    send_first(0, row, r1.at[0])
    perm[...] = perm_f32.T.astype(BF16)

    @pl.when(y != 2)
    def _():
        arrived(ig.at[pl.ds(0, 2 * EDGE)], re.at[0])

    convolve_chip((y + 1) % SIDE)
    convolve_chip(y)
    send_mixer(1)
    recvm[tp] = normed[pl.ds(pl.multiple_of(tp * tokens, tokens), tokens), :]

    chunk_in = PER_CHUNK * GROUP_ROWS
    chunk_out = TP * GROUP_ROWS

    def places(j):
        info = recv1[j * chunk_in : (j + 1) * chunk_in, 0:META].astype(F32)
        shift = ((iota((chunk_in, chunk_out), 0) >> 4) * EXPERT_ROWS).astype(F32)
        lane = iota((chunk_in, chunk_out), 1).astype(F32)
        return info, info[:, 0:1] + shift == lane, info[:, 1:2] + shift == lane

    def send_second(j, cols):
        for q in TP_ORDER:
            rows = pl.ds(j * chunk_out + q * GROUP_ROWS, GROUP_ROWS)
            send(send2.at[rows, cols], recv2.at[rows, cols], sent_sem.at[1], r2.at[j], tp_peer(q))

    def split_tile(j, split, cols):
        base = j * chunk_out
        moved = dot(split, recv1[j * chunk_in : (j + 1) * chunk_in, shifted(cols)]).astype(BF16)
        send2[base : base + chunk_out, cols] = moved
        recv2[base : base + GROUP_ROWS, cols] = moved[0:GROUP_ROWS]

    def splitter(j):
        _, at0, at1 = places(j)
        return (hot(at0) + hot(at1)).T.astype(BF16)

    others = pl.ds((NEAR * PER_CHUNK + 1) * GROUP_ROWS, (PER_CHUNK - 1) * GROUP_ROWS)
    whole = pl.ds(0, width)
    out_halves = (pl.ds(0, width // 2), pl.ds(width // 2, width // 2))
    arrived(recv1.at[others, halves[0]], r1.at[NEAR])
    split = splitter(NEAR)
    for cols in tiles[:half]:
        split_tile(NEAR, split, cols)
    send_second(NEAR, out_halves[0])
    arrived(recv1.at[others, halves[1]], r1.at[CHUNKS])
    for cols in tiles[half:]:
        split_tile(NEAR, split, cols)
    send_second(NEAR, out_halves[1])
    send_first(1, row, r1.at[1])
    convolve_chip((y + 3) % SIDE)
    for j in range(NEAR):
        arrived(recv1.at[pl.ds(j * chunk_in, chunk_in)], r1.at[j])
        if j == 0:
            send_first(2, row, r1.at[2])
        split = splitter(j)
        for cols in tiles:
            split_tile(j, split, cols)
        send_second(j, whole)

    ld_wg.wait()
    ld_wu.wait()
    ld_wd.wait()
    hidden_units = wg.shape[1]
    hid_tile = 256

    def send_third(j, cols, sem):
        for q in TP_ORDER:
            rows = pl.ds(j * chunk_out + q * GROUP_ROWS, GROUP_ROWS)
            send(send3.at[rows, cols], res.at[rows, cols], sent_sem.at[2], sem, tp_peer(q, back=True))

    for j in range(CHUNKS):
        base = j * chunk_out
        arrived(recv2.at[pl.ds(base + GROUP_ROWS, chunk_out - GROUP_ROWS)], r2.at[j])

        @pl.loop(0, hidden_units // hid_tile)
        def _(n):
            cols = pl.ds(pl.multiple_of(n * hid_tile, hid_tile), hid_tile)
            inputs = recv2[base : base + chunk_out, :]
            gate = dot(inputs, wg[:, cols])
            up = dot(inputs, wu[:, cols])
            hid[:, cols] = (gate / (1.0 + jnp.exp(-gate)) * up).astype(BF16)

        def down(n):
            cols = pl.ds(pl.multiple_of(n * tile, tile), tile)
            result = dot(hid[...], wd[:, cols]).astype(BF16)
            send3[base : base + chunk_out, cols] = result
            res[base : base + GROUP_ROWS, cols] = result[0:GROUP_ROWS]

        if j < NEAR:
            pl.loop(0, len(tiles))(down)
            send_third(j, whole, r3.at[j])
        else:
            pl.loop(0, half)(down)
            send_third(j, out_halves[0], r3.at[NEAR])
            pl.loop(half, len(tiles))(down)
            send_third(j, out_halves[1], r3.at[CHUNKS])
    send_mixer(2)

    def chip_part(dy, cols):
        chip = (y + dy) % SIDE
        pair = jnp.concatenate([recvm[chip * 2], recvm[chip * 2 + 1]], axis=1)
        weights = mixw[pl.ds(pl.multiple_of(chip * (2 * META), 2 * META), 2 * META), cols]
        return dot(pair, weights)

    ld_mw.wait()
    for group in (0, 1):
        arrived(recvm.at[pl.ds(0, len(MIX_GROUPS[group]))], rm.at[group])

    @pl.loop(0, len(tiles))
    def _(n):
        cols = pl.ds(pl.multiple_of(n * tile, tile), tile)
        mixed_sum[:, cols] = chip_part(0, cols) + chip_part(2, cols) + chip_part(3, cols)

    def weights_of(j):
        info, at0, at1 = places(j)
        high = jnp.where(at0, info[:, 2:3], 0.0) + jnp.where(at1, info[:, 4:5], 0.0)
        low = jnp.where(at0, info[:, 3:4], 0.0) + jnp.where(at1, info[:, 5:6], 0.0)
        return high.astype(BF16), low.astype(BF16)

    def join_tile(j, high, low, cols):
        base = j * chunk_in
        results = res[j * chunk_out : (j + 1) * chunk_out, cols]
        joined = (dot(high, results) + dot(low, results)).astype(BF16)
        send4[base : base + chunk_in, cols] = joined
        if j == NEAR:
            ret[mine, cols] = joined[mine.start - near.start : mine.stop - near.start]

    def send_home(j, cols):
        for k in chunk_peers(j):
            dz, dx = OFFSETS[k]
            rows = pl.ds(k * GROUP_ROWS, GROUP_ROWS)
            peer = ep_peer(SIDE - dz, SIDE - dx)
            send(send4.at[rows, cols], ret.at[rows, cols], sent_sem.at[3], r4.at[0], peer)

    for j in range(NEAR):
        high, low = weights_of(j)
        base = j * chunk_out
        arrived(res.at[pl.ds(base + GROUP_ROWS, chunk_out - GROUP_ROWS)], r3.at[j])
        for cols in tiles:
            join_tile(j, high, low, cols)
        send_home(j, whole)
    high, low = weights_of(NEAR)
    rows = pl.ds(NEAR * chunk_out + GROUP_ROWS, chunk_out - GROUP_ROWS)
    arrived(res.at[rows, out_halves[0]], r3.at[NEAR])
    for cols in tiles[:half]:
        join_tile(NEAR, high, low, cols)
    send_home(NEAR, out_halves[0])
    arrived(res.at[rows, out_halves[1]], r3.at[CHUNKS])
    for cols in tiles[half:]:
        join_tile(NEAR, high, low, cols)
    send_home(NEAR, out_halves[1])

    arrived(recvm.at[pl.ds(0, len(MIX_GROUPS[2]))], rm.at[2])
    for cols in tiles:
        mixed[:, cols] = (mixed_sum[:, cols] + chip_part(1, cols)).astype(BF16)

    remote_rows = pl.ds(0, (EP - 1) * GROUP_ROWS)
    remote_slots = pl.ds(0, CHUNKS * (chunk_out - GROUP_ROWS))
    departed(send1.at[remote_rows], sent_sem.at[0])
    departed(send2.at[remote_slots], sent_sem.at[1])
    departed(send3.at[remote_slots], sent_sem.at[2])
    departed(recvm.at[pl.ds(0, TP - 1)], sent_sem.at[4])
    departed(ig.at[pl.ds(0, 2 * EDGE)], sent_sem.at[5])
    departed(send4.at[remote_rows], sent_sem.at[3])
    arrived(send4.at[remote_rows], r4.at[0])


def finish(perm, ret, mixed, out_mixed, out_moe, moe, sem):
    width = ret.shape[1]
    steps = sem.shape[0] - 1
    tile = width // steps
    mixed_out = pltpu.make_async_copy(mixed, out_mixed, sem.at[steps])
    mixed_out.start()
    outs = []
    for n in range(steps):
        cols = slice(n * tile, (n + 1) * tile)
        moe[:, cols] = dot(perm[...], ret[:, cols]).astype(BF16)
        outs.append(pltpu.make_async_copy(moe.at[:, cols], out_moe.at[:, cols], sem.at[n]))
        outs[-1].start()
    for cp in outs:
        cp.wait()
    mixed_out.wait()


def shards(
    out_gate, in_gate, conv_input, conv_taps, group_gain, mix_out_w, moe_in, moe_gain, route_ids, route_weight,
    gate_w, up_w, down_w,
):
    rows, channels = in_gate.shape
    tokens, width = moe_in.shape
    hidden = gate_w.shape[2]
    hbm = pl.BlockSpec(memory_space=pltpu.HBM)
    vmem = pl.BlockSpec(memory_space=pltpu.VMEM)
    dma = pltpu.SemaphoreType.DMA
    V = pltpu.VMEM
    out = jax.ShapeDtypeStruct((tokens, width), BF16)
    square = jax.ShapeDtypeStruct((tokens, tokens), BF16)
    slots = 2 * tokens
    mixed, returned, perm = pl.pallas_call(
        kernel,
        out_shape=(out, out, square),
        in_specs=[hbm] * 13,
        out_specs=(vmem, vmem, vmem),
        scratch_shapes=[
            V(conv_taps.shape, F32),
            V((1, channels), F32),
            V((1, width), F32),
            V((2, tokens), jnp.int32),
            V((2, tokens), F32),
            V((tokens, width), BF16),
            V((tokens, width), BF16),
            V((rows, channels), BF16),
            V((rows + EDGE, channels), BF16),
            V((rows + EDGE, channels), BF16),
            V((rows, channels), BF16),
            V((TP, tokens, channels), BF16),
            V(mix_out_w.shape, BF16),
            V((width, hidden), BF16),
            V((width, hidden), BF16),
            V((hidden, width), BF16),
            V((tokens, META + width), BF16),
            V((tokens, META + width), BF16),
            V((slots, width), BF16),
            V((slots, width), BF16),
            V((TP * GROUP_ROWS, hidden), BF16),
            V((slots, width), BF16),
            V((slots, width), BF16),
            V((tokens, width), BF16),
            V((tokens, width), F32),
            dma((13,)),
            dma((6,)),
            dma((CHUNKS + 1,)),
            dma((CHUNKS,)),
            dma((CHUNKS + 1,)),
            dma((1,)),
            dma((len(MIX_GROUPS),)),
            dma((1,)),
        ],
        compiler_params=pltpu.CompilerParams(
            collective_id=0, has_side_effects=True, vmem_limit_bytes=48 * 1024 * 1024
        ),
    )(*[
        pltpu.with_memory_space_constraint(array, pltpu.HBM)
        for array in (
            conv_taps, group_gain.reshape(1, -1), moe_gain.reshape(1, -1), route_ids.T, route_weight.T,
            out_gate, in_gate, conv_input, mix_out_w, moe_in, gate_w, up_w, down_w,
        )
    ])
    return pl.pallas_call(
        finish,
        out_shape=(out, out),
        in_specs=[vmem] * 3,
        out_specs=(hbm, hbm),
        scratch_shapes=[V((tokens, width), BF16), dma((5,))],
        compiler_params=pltpu.CompilerParams(vmem_limit_bytes=12 * 1024 * 1024),
    )(perm, returned, mixed)


def solution(mesh):
    both = ("ep", "tp")
    in_specs = (
        P("ep", "tp"), P("ep", "tp"), P("ep", "tp"), P(None, "tp"), P("tp"), P(),
        P(both, None), P(), P(both, None), P(both, None),
        P(both, None, None), P(both, None, None), P(both, None, None),
    )
    return jax.shard_map(
        shards, mesh=mesh, in_specs=in_specs, out_specs=(P(both, None), P(both, None)), check_vma=False
    )
```

```python
import functools

import jax
import jax.numpy as jnp
from jax import lax
from jax.experimental import pallas as pl
from jax.experimental.pallas import tpu as pltpu
from jax.sharding import PartitionSpec as P

MESH = pl.DeviceIdType.MESH
F32 = jnp.float32
BF16 = jnp.bfloat16
EPS = 1e-06

SIDE = 4
ORDER = (
    ((1, 2), (2, 1), (0, 2), (2, 0)),
    ((2, 2), (2, 3), (3, 2), (1, 1)),
    ((3, 0), (1, 3), (3, 1), (3, 3)),
    ((0, 0), (0, 1), (1, 0), (0, 3)),
)
OFFSETS = tuple(pair for chunk in ORDER for pair in chunk)
CHUNKS = len(ORDER)
SELF = OFFSETS.index((0, 0))
SPLIT_ORDER = (3, 0, 1, 2)
PER_CHUNK = len(ORDER[0])
EP = len(OFFSETS)
TP = 8
GROUP_ROWS = 16
EXPERT_ROWS = 4
META = 128
GROUP_CH = 64
TP_ORDER = (4, 5, 2, 3, 6, 7, 1)
MIX_GROUPS = ((4, 5), (1,), (2, 3, 6, 7))
NEAR = CHUNKS - 1
EDGE = 16


def chunk_peers(j):
    return [k for k in range(j * PER_CHUNK, (j + 1) * PER_CHUNK) if k != SELF]


def iota(shape, dim):
    return lax.broadcasted_iota(jnp.int32, shape, dim)


def hot(mask):
    return jnp.where(mask, 1.0, 0.0)


def dot(a, b, contract=((1,), (0,))):
    return lax.dot_general(a, b, (contract, ((), ())), preferred_element_type=F32)


def kernel(
    taps_hbm, ggain_hbm, mgain_hbm, ids_hbm, rw_hbm, og_hbm, ig_hbm, ci_hbm, mixw_hbm, x_hbm, wg_hbm, wu_hbm, wd_hbm,
    mixed, ret, perm,
    taps_ref, ggain_ref, mgain_ref, ids_ref, rw_ref,
    x_buf, xn_buf, og, ig, ci, normed, recvm, mixw, wg, wu, wd,
    send1, recv1, send2, recv2, hid, send3, res, send4, mixed_sum,
    load_sem, sent_sem, r1, r2, r3, r4, rm, re,
):
    ep = lax.axis_index("ep")
    tp = lax.axis_index("tp")
    z, x = ep // SIDE, ep % SIDE
    y, c = tp // 2, tp % 2
    tokens, width = x_buf.shape
    length = og.shape[0]

    def ep_peer(dz, dx):
        return (((z + dz) % SIDE) * SIDE + (x + dx) % SIDE, tp)

    def tp_peer(q, back=False):
        dy, dc = q // 2, q % 2
        dy = SIDE - dy if back else dy
        return (ep, ((y + dy) % SIDE) * 2 + (c + dc) % 2)

    def load(i, src, dst):
        cp = pltpu.make_async_copy(src, dst, load_sem.at[i])
        cp.start()
        return cp

    ld_ids = load(8, ids_hbm, ids_ref)
    ld_rw = load(9, rw_hbm, rw_ref)
    inner = pl.ds(EDGE, length)
    ld_ig = load(1, ig_hbm, ig.at[inner])
    ld_ci = load(2, ci_hbm, ci.at[inner])
    ld_og = load(3, og_hbm, og)
    ld_taps = load(11, taps_hbm, taps_ref)
    ld_ggain = load(12, ggain_hbm, ggain_ref)
    ld_x = load(0, x_hbm, x_buf)
    ld_mgain = load(10, mgain_hbm, mgain_ref)

    barrier = pltpu.get_barrier_semaphore()
    for k in range(EP):
        if k == SELF:
            continue
        dz, dx = OFFSETS[k]
        pl.semaphore_signal(barrier, inc=1, device_id=ep_peer(dz, dx), device_id_type=MESH)
    for q in range(1, TP):
        pl.semaphore_signal(barrier, inc=1, device_id=tp_peer(q), device_id_type=MESH)

    def send(src, dst, ssem, rsem, device):
        pltpu.make_async_remote_copy(
            src_ref=src, dst_ref=dst, send_sem=ssem, recv_sem=rsem, device_id=device, device_id_type=MESH
        ).start()

    def arrived(ref, sem):
        pltpu.make_async_remote_copy(
            src_ref=ref, dst_ref=ref, send_sem=sem, recv_sem=sem, device_id=tp_peer(1), device_id_type=MESH
        ).wait_recv()

    def departed(ref, sem):
        pltpu.make_async_remote_copy(
            src_ref=ref, dst_ref=ref, send_sem=sem, recv_sem=sem, device_id=tp_peer(1), device_id_type=MESH
        ).wait_send()

    ld_ids.wait()
    ld_rw.wait()
    id0 = ids_ref[0:1, :]
    id1 = ids_ref[1:2, :]
    earlier = hot(iota((tokens, tokens), 0) < iota((tokens, tokens), 1)).astype(BF16)
    expert_of = iota((EP * TP, tokens), 0)
    hits0 = hot(expert_of == id0)
    hits1 = hot(expert_of == id1)
    before = dot((hits0 + hits1).astype(BF16), earlier)
    rank0 = jnp.sum(hits0 * before, axis=0, keepdims=True)
    rank1 = jnp.sum(hits1 * before, axis=0, keepdims=True)

    def base_slot(ids, rank):
        inner = ids & (TP - 1)
        dy = ((inner >> 1) - y) & (SIDE - 1)
        dc = ((inner & 1) + c) & 1
        return ((dy * 2 + dc) * GROUP_ROWS).astype(F32) + rank

    base0 = base_slot(id0, rank0)
    base1 = base_slot(id1, rank1)
    group = id0 >> 3
    place = (((group >> 2) - z) & 3) * SIDE + (((group & 3) - x) & 3)
    order = jnp.zeros_like(place)
    for k, (dz, dx) in enumerate(OFFSETS):
        order = jnp.where(place == dz * SIDE + dx, k, order)
    members = hot(iota((EP, tokens), 0) == order)
    group_rank = jnp.sum(members * dot(members.astype(BF16), earlier), axis=0, keepdims=True)
    slot = (order * GROUP_ROWS).astype(F32) + group_rank
    perm_f32 = hot(iota((tokens, tokens), 0).astype(F32) == slot)
    forward = perm_f32.astype(BF16)
    w_hi = rw_ref[...].astype(BF16).astype(F32)
    w_lo = rw_ref[...] - w_hi
    meta_rows = jnp.concatenate(
        [base0, base1, w_hi[0:1], w_lo[0:1], w_hi[1:2], w_lo[1:2], jnp.zeros((META - 6, tokens), F32)], axis=0
    )
    meta = dot(forward, meta_rows.astype(BF16), ((1,), (1,))).astype(BF16)
    mine = slice(SELF * GROUP_ROWS, (SELF + 1) * GROUP_ROWS)
    send1[:, 0:META] = meta
    recv1[mine, 0:META] = meta[mine]

    ld_ig.wait()
    ld_ci.wait()
    pl.semaphore_wait(barrier, EP - 1 + TP - 1)
    after = (lax.rem(ep + 1, EP), tp)
    for ref in (ig, ci):
        send(ref.at[pl.ds(length, EDGE)], ref.at[pl.ds(0, EDGE)], sent_sem.at[5], re.at[0], after)

    ld_og.wait()
    ld_taps.wait()
    ld_ggain.wait()
    same = hot((iota((META, META), 0) >> 6) == (iota((META, META), 1) >> 6))
    averager = (same * (1.0 / GROUP_CH)).astype(BF16)

    def convolve(i):
        rows = pl.ds(pl.multiple_of(i * tokens, tokens), tokens)
        wide = pl.ds(pl.multiple_of(i * tokens, EDGE), tokens + EDGE)
        block = ig[wide, :].astype(F32) * ci[wide, :].astype(F32)
        keep = jnp.where(ep * TP + i > 0, 1.0, 0.0)
        block = jnp.concatenate([block[0:EDGE] * keep, block[EDGE:]], axis=0)
        convolved = (
            taps_ref[0:1, :] * pltpu.roll(block, 2, 0)[EDGE:]
            + taps_ref[1:2, :] * pltpu.roll(block, 1, 0)[EDGE:]
            + taps_ref[2:3, :] * block[EDGE:]
        )
        gated = og[rows, :].astype(F32) * convolved
        square = gated * gated
        high = square.astype(BF16)
        low = (square - high.astype(F32)).astype(BF16)
        inv = lax.rsqrt(dot(high, averager) + dot(low, averager) + EPS)
        normed[rows, :] = (gated * inv * ggain_ref[...]).astype(BF16)

    def convolve_chip(chip):
        convolve(chip * 2)
        convolve(chip * 2 + 1)

    def send_mixer(group):
        for q in MIX_GROUPS[group]:
            peer = tp_peer(q)
            rows = pl.ds(pl.multiple_of(peer[1] * tokens, tokens), tokens)
            send(normed.at[rows], recvm.at[tp], sent_sem.at[4], rm.at[group], peer)

    @pl.when(y != 2)
    def _():
        convolve_chip((y + 2) % SIDE)
        send_mixer(0)

    ld_x.wait()
    ld_mgain.wait()
    ld_wg = load(4, wg_hbm.at[0], wg)
    ld_wu = load(5, wu_hbm.at[0], wu)
    ld_wd = load(6, wd_hbm.at[0], wd)
    ld_mw = load(7, mixw_hbm, mixw)
    wide_in = x_buf[...].astype(F32)
    scale = lax.rsqrt(jnp.mean(wide_in * wide_in, axis=-1, keepdims=True) + EPS)
    tile = 512
    tiles = [slice(n * tile, (n + 1) * tile) for n in range(width // tile)]
    half = len(tiles) // 2
    near = slice(NEAR * PER_CHUNK * GROUP_ROWS, tokens)
    halves = (pl.ds(0, META + width // 2), pl.ds(META + width // 2, width // 2))

    def shifted(cols):
        return slice(cols.start + META, cols.stop + META)

    def send_first(j, cols, sem):
        for k in chunk_peers(j):
            rows = pl.ds(k * GROUP_ROWS, GROUP_ROWS)
            send(send1.at[rows, cols], recv1.at[rows, cols], sent_sem.at[0], sem, ep_peer(*OFFSETS[k]))

    for n, cols in enumerate(tiles):
        tile_in = (x_buf[:, cols].astype(F32) * scale * mgain_ref[:, cols]).astype(BF16)
        xn_buf[:, cols] = tile_in
        moved = dot(forward[near], tile_in).astype(BF16)
        send1[near, shifted(cols)] = moved
        recv1[mine, shifted(cols)] = moved[mine.start - near.start : mine.stop - near.start]
        if n == half - 1:
            send_first(NEAR, halves[0], r1.at[NEAR])
    send_first(NEAR, halves[1], r1.at[CHUNKS])
    far = slice(0, near.start)
    for cols in tiles:
        send1[far, shifted(cols)] = dot(forward[far], xn_buf[:, cols]).astype(BF16)
    row = pl.ds(0, META + width)
    send_first(0, row, r1.at[0])
    perm[...] = perm_f32.T.astype(BF16)

    arrived(ig.at[pl.ds(0, 2 * EDGE)], re.at[0])

    @pl.when(y == 2)
    def _():
        convolve_chip((y + 2) % SIDE)
        send_mixer(0)

    convolve_chip(y)
    send_mixer(1)
    recvm[tp] = normed[pl.ds(pl.multiple_of(tp * tokens, tokens), tokens), :]

    chunk_in = PER_CHUNK * GROUP_ROWS
    chunk_out = TP * GROUP_ROWS

    def places(j):
        info = recv1[j * chunk_in : (j + 1) * chunk_in, 0:META].astype(F32)
        shift = ((iota((chunk_in, chunk_out), 0) >> 4) * EXPERT_ROWS).astype(F32)
        lane = iota((chunk_in, chunk_out), 1).astype(F32)
        return info, info[:, 0:1] + shift == lane, info[:, 1:2] + shift == lane

    def send_second(j, cols):
        for q in TP_ORDER:
            rows = pl.ds(j * chunk_out + q * GROUP_ROWS, GROUP_ROWS)
            send(send2.at[rows, cols], recv2.at[rows, cols], sent_sem.at[1], r2.at[j], tp_peer(q))

    def split_tile(j, split, cols):
        base = j * chunk_out
        moved = dot(split, recv1[j * chunk_in : (j + 1) * chunk_in, shifted(cols)]).astype(BF16)
        send2[base : base + chunk_out, cols] = moved
        recv2[base : base + GROUP_ROWS, cols] = moved[0:GROUP_ROWS]

    def splitter(j):
        _, at0, at1 = places(j)
        return (hot(at0) + hot(at1)).T.astype(BF16)

    others = pl.ds((NEAR * PER_CHUNK + 1) * GROUP_ROWS, (PER_CHUNK - 1) * GROUP_ROWS)
    whole = pl.ds(0, width)
    out_halves = (pl.ds(0, width // 2), pl.ds(width // 2, width // 2))
    arrived(recv1.at[others, halves[0]], r1.at[NEAR])
    split = splitter(NEAR)
    for cols in tiles[:half]:
        split_tile(NEAR, split, cols)
    send_second(NEAR, out_halves[0])
    arrived(recv1.at[others, halves[1]], r1.at[CHUNKS])
    for cols in tiles[half:]:
        split_tile(NEAR, split, cols)
    send_second(NEAR, out_halves[1])
    send_first(1, row, r1.at[1])
    convolve_chip((y + 1) % SIDE)
    convolve_chip((y + 3) % SIDE)
    for j in range(NEAR):
        arrived(recv1.at[pl.ds(j * chunk_in, chunk_in)], r1.at[j])
        if j == 0:
            send_first(2, row, r1.at[2])
        split = splitter(j)
        for cols in tiles:
            split_tile(j, split, cols)
        send_second(j, whole)

    ld_wg.wait()
    ld_wu.wait()
    ld_wd.wait()
    hidden_units = wg.shape[1]
    hid_tile = 256

    def send_third(j, cols, sem):
        for q in TP_ORDER:
            rows = pl.ds(j * chunk_out + q * GROUP_ROWS, GROUP_ROWS)
            send(send3.at[rows, cols], res.at[rows, cols], sent_sem.at[2], sem, tp_peer(q, back=True))

    for j in range(CHUNKS):
        base = j * chunk_out
        arrived(recv2.at[pl.ds(base + GROUP_ROWS, chunk_out - GROUP_ROWS)], r2.at[j])

        @pl.loop(0, hidden_units // hid_tile)
        def _(n):
            cols = pl.ds(pl.multiple_of(n * hid_tile, hid_tile), hid_tile)
            inputs = recv2[base : base + chunk_out, :]
            gate = dot(inputs, wg[:, cols])
            up = dot(inputs, wu[:, cols])
            hid[:, cols] = (gate / (1.0 + jnp.exp(-gate)) * up).astype(BF16)

        def down(n):
            cols = pl.ds(pl.multiple_of(n * tile, tile), tile)
            result = dot(hid[...], wd[:, cols]).astype(BF16)
            send3[base : base + chunk_out, cols] = result
            res[base : base + GROUP_ROWS, cols] = result[0:GROUP_ROWS]

        if j < NEAR:
            pl.loop(0, len(tiles))(down)
            send_third(j, whole, r3.at[j])
        else:
            pl.loop(0, half)(down)
            send_third(j, out_halves[0], r3.at[NEAR])
            pl.loop(half, len(tiles))(down)
            send_third(j, out_halves[1], r3.at[CHUNKS])

    def chip_part(dy, cols):
        chip = (y + dy) % SIDE
        pair = jnp.concatenate([recvm[chip * 2], recvm[chip * 2 + 1]], axis=1)
        weights = mixw[pl.ds(pl.multiple_of(chip * (2 * META), 2 * META), 2 * META), cols]
        return dot(pair, weights)

    ld_mw.wait()
    for group in (0, 1):
        arrived(recvm.at[pl.ds(0, len(MIX_GROUPS[group]))], rm.at[group])

    @pl.loop(0, len(tiles))
    def _(n):
        cols = pl.ds(pl.multiple_of(n * tile, tile), tile)
        mixed_sum[:, cols] = chip_part(0, cols) + chip_part(2, cols)

    def weights_of(j):
        info, at0, at1 = places(j)
        high = jnp.where(at0, info[:, 2:3], 0.0) + jnp.where(at1, info[:, 4:5], 0.0)
        low = jnp.where(at0, info[:, 3:4], 0.0) + jnp.where(at1, info[:, 5:6], 0.0)
        return high.astype(BF16), low.astype(BF16)

    def join_tile(j, high, low, cols):
        base = j * chunk_in
        results = res[j * chunk_out : (j + 1) * chunk_out, cols]
        joined = (dot(high, results) + dot(low, results)).astype(BF16)
        send4[base : base + chunk_in, cols] = joined
        if j == NEAR:
            ret[mine, cols] = joined[mine.start - near.start : mine.stop - near.start]

    def send_home(j, cols):
        for k in chunk_peers(j):
            dz, dx = OFFSETS[k]
            rows = pl.ds(k * GROUP_ROWS, GROUP_ROWS)
            peer = ep_peer(SIDE - dz, SIDE - dx)
            send(send4.at[rows, cols], ret.at[rows, cols], sent_sem.at[3], r4.at[0], peer)

    for j in range(NEAR):
        high, low = weights_of(j)
        base = j * chunk_out
        arrived(res.at[pl.ds(base + GROUP_ROWS, chunk_out - GROUP_ROWS)], r3.at[j])
        for cols in tiles:
            join_tile(j, high, low, cols)
        send_home(j, whole)
    send_mixer(2)
    high, low = weights_of(NEAR)
    rows = pl.ds(NEAR * chunk_out + GROUP_ROWS, chunk_out - GROUP_ROWS)
    arrived(res.at[rows, out_halves[0]], r3.at[NEAR])
    for cols in tiles[:half]:
        join_tile(NEAR, high, low, cols)
    send_home(NEAR, out_halves[0])
    arrived(res.at[rows, out_halves[1]], r3.at[CHUNKS])
    for cols in tiles[half:]:
        join_tile(NEAR, high, low, cols)
    send_home(NEAR, out_halves[1])

    arrived(recvm.at[pl.ds(0, len(MIX_GROUPS[2]))], rm.at[2])
    for cols in tiles:
        mixed[:, cols] = (mixed_sum[:, cols] + chip_part(1, cols) + chip_part(3, cols)).astype(BF16)

    remote_rows = pl.ds(0, (EP - 1) * GROUP_ROWS)
    remote_slots = pl.ds(0, CHUNKS * (chunk_out - GROUP_ROWS))
    departed(send1.at[remote_rows], sent_sem.at[0])
    departed(send2.at[remote_slots], sent_sem.at[1])
    departed(send3.at[remote_slots], sent_sem.at[2])
    departed(recvm.at[pl.ds(0, TP - 1)], sent_sem.at[4])
    departed(ig.at[pl.ds(0, 2 * EDGE)], sent_sem.at[5])
    departed(send4.at[remote_rows], sent_sem.at[3])
    arrived(send4.at[remote_rows], r4.at[0])


def finish(perm, ret, mixed, out_mixed, out_moe, moe, sem):
    width = ret.shape[1]
    steps = sem.shape[0] - 1
    tile = width // steps
    mixed_out = pltpu.make_async_copy(mixed, out_mixed, sem.at[steps])
    mixed_out.start()
    outs = []
    for n in range(steps):
        cols = slice(n * tile, (n + 1) * tile)
        moe[:, cols] = dot(perm[...], ret[:, cols]).astype(BF16)
        outs.append(pltpu.make_async_copy(moe.at[:, cols], out_moe.at[:, cols], sem.at[n]))
        outs[-1].start()
    for cp in outs:
        cp.wait()
    mixed_out.wait()


def shards(
    out_gate, in_gate, conv_input, conv_taps, group_gain, mix_out_w, moe_in, moe_gain, route_ids, route_weight,
    gate_w, up_w, down_w,
):
    rows, channels = in_gate.shape
    tokens, width = moe_in.shape
    hidden = gate_w.shape[2]
    hbm = pl.BlockSpec(memory_space=pltpu.HBM)
    vmem = pl.BlockSpec(memory_space=pltpu.VMEM)
    dma = pltpu.SemaphoreType.DMA
    V = pltpu.VMEM
    out = jax.ShapeDtypeStruct((tokens, width), BF16)
    square = jax.ShapeDtypeStruct((tokens, tokens), BF16)
    slots = 2 * tokens
    mixed, returned, perm = pl.pallas_call(
        kernel,
        out_shape=(out, out, square),
        in_specs=[hbm] * 13,
        out_specs=(vmem, vmem, vmem),
        scratch_shapes=[
            V(conv_taps.shape, F32),
            V((1, channels), F32),
            V((1, width), F32),
            V((2, tokens), jnp.int32),
            V((2, tokens), F32),
            V((tokens, width), BF16),
            V((tokens, width), BF16),
            V((rows, channels), BF16),
            V((rows + EDGE, channels), BF16),
            V((rows + EDGE, channels), BF16),
            V((rows, channels), BF16),
            V((TP, tokens, channels), BF16),
            V(mix_out_w.shape, BF16),
            V((width, hidden), BF16),
            V((width, hidden), BF16),
            V((hidden, width), BF16),
            V((tokens, META + width), BF16),
            V((tokens, META + width), BF16),
            V((slots, width), BF16),
            V((slots, width), BF16),
            V((TP * GROUP_ROWS, hidden), BF16),
            V((slots, width), BF16),
            V((slots, width), BF16),
            V((tokens, width), BF16),
            V((tokens, width), F32),
            dma((13,)),
            dma((6,)),
            dma((CHUNKS + 1,)),
            dma((CHUNKS,)),
            dma((CHUNKS + 1,)),
            dma((1,)),
            dma((len(MIX_GROUPS),)),
            dma((1,)),
        ],
        compiler_params=pltpu.CompilerParams(
            collective_id=0, has_side_effects=True, vmem_limit_bytes=48 * 1024 * 1024
        ),
    )(*[
        pltpu.with_memory_space_constraint(array, pltpu.HBM)
        for array in (
            conv_taps, group_gain.reshape(1, -1), moe_gain.reshape(1, -1), route_ids.T, route_weight.T,
            out_gate, in_gate, conv_input, mix_out_w, moe_in, gate_w, up_w, down_w,
        )
    ])
    return pl.pallas_call(
        finish,
        out_shape=(out, out),
        in_specs=[vmem] * 3,
        out_specs=(hbm, hbm),
        scratch_shapes=[V((tokens, width), BF16), dma((5,))],
        compiler_params=pltpu.CompilerParams(vmem_limit_bytes=12 * 1024 * 1024),
    )(perm, returned, mixed)


def solution(mesh):
    both = ("ep", "tp")
    in_specs = (
        P("ep", "tp"), P("ep", "tp"), P("ep", "tp"), P(None, "tp"), P("tp"), P(),
        P(both, None), P(), P(both, None), P(both, None),
        P(both, None, None), P(both, None, None), P(both, None, None),
    )
    return jax.shard_map(
        shards, mesh=mesh, in_specs=in_specs, out_specs=(P(both, None), P(both, None)), check_vma=False
    )
```
